32 devices in a mesh: kv: 8 (over z, y), tp: 4 (over x, core).
Axes of the slice: x: 2, y: 2, z: 4, core: 2. Of those that a mesh axis runs over, the one named last changes fastest.
Arguments:
- tokens: bfloat16 [16, 4096], P(None, ('kv', 'tp')), may hold values from -17 to 17
- first_gain: float32 [4096], P('kv'), may hold values from 0.1 to 1.9
- first_gate: bfloat16 [4096, 11264], P('kv', 'tp'), may hold values from -0.09375 to 0.09375
- first_up: bfloat16 [4096, 11264], P('kv', 'tp'), may hold values from -0.09375 to 0.09375
- first_down: bfloat16 [11264, 4096], P('tp', 'kv'), may hold values from -0.0546875 to 0.0546875
- mixer_gain: float32 [4096], P('kv'), may hold values from 0.1 to 1.9
- w_query: bfloat16 [4096, 4096], P('kv', 'tp'), may hold values from -0.09375 to 0.09375
- w_key: bfloat16 [4096, 4096], P('kv', 'tp'), may hold values from -0.328125 to 0.328125
- w_value: bfloat16 [4096, 4096], P('kv', 'tp'), may hold values from -0.09375 to 0.09375
- w_output: bfloat16 [4096, 4096], P('tp', 'kv'), may hold values from -0.09375 to 0.09375
- lam_heads: float32 [32], P('tp'), may hold values from 0.3 to 0.8
- head_gain: float32 [128], replicated, may hold values from 0.1 to 1.9
- key_cache: bfloat16 [16, 2048, 32, 128], P(None, 'kv', 'tp'), may hold values from -1000 to 1000
- value_cache: bfloat16 [16, 2048, 32, 128], P(None, 'kv', 'tp'), may hold values from -6 to 6
- lengths: int32 [16], replicated, may hold values from 1 to 2048, 12288 in all
- last_gain: float32 [4096], P('kv'), may hold values from 0.1 to 1.9
- last_gate: bfloat16 [4096, 11264], P('kv', 'tp'), may hold values from -0.09375 to 0.09375
- last_up: bfloat16 [4096, 11264], P('kv', 'tp'), may hold values from -0.09375 to 0.09375
- last_down: bfloat16 [11264, 4096], P('tp', 'kv'), may hold values from -0.0546875 to 0.0546875
Outputs:
- result: bfloat16 [16, 4096], P(None, ('kv', 'tp'))
The draws below stay inside these ranges and needn't reach their ends.
Inputs may be any that keep to these rules, and one draw needn't show every extreme that they name: Sequence b reads cached positions 0 to lengths[b] - 1 and its new token.
All inputs are finite; a program needn't handle non-finite values.
Results may differ from the reference program's by a relative error of at most 0.04.
Values may be sent and summed in bfloat16 or wider, within the bound.
A program may use at most 128 MiB of HBM per device.

```python
import math
import jax
import jax.numpy as jnp
import numpy as np
from jax import lax

WIDTH = 4096
HEADS = 32
HEAD_DIM = 64
VAL_DIM = 128
FFN_UNITS = 11264
BATCH = 16
SEQ_LEN = 2048


def draw_tokens(key, part):
    base = jnp.clip(jax.random.normal(jax.random.fold_in(key, 11), (BATCH, WIDTH), jnp.float32), -6.0, 6.0)
    column = jnp.arange(WIDTH, dtype=jnp.float32) / (WIDTH - 1)
    logit_scale = 0.6 * jnp.exp(jnp.log(4.0) * column)[None, :]
    return (base * logit_scale).astype(jnp.bfloat16)


def draw_key_cache(key, part):
    shape = (BATCH, SEQ_LEN, HEADS, 2 * HEAD_DIM)
    base = 1.75 * jnp.clip(jax.random.normal(jax.random.fold_in(key, 21), shape, jnp.float32), -8.0, 8.0)
    return base.astype(jnp.bfloat16)


def block_levels(rng, dims, split, low, top_value):
    def one(axis_at, parts):
        steps = jax.random.uniform(jax.random.fold_in(jax.random.fold_in(rng, 6), axis_at), (parts,), jnp.float32, low / len(split), top_value / len(split))
        return jnp.repeat(jnp.exp(steps), dims[axis_at] // parts).reshape((-1,) + (1,) * (len(dims) - axis_at - 1))

    loudness = one(*split[0])
    for cut in split[1:]:
        loudness = loudness * one(*cut)
    return loudness


def length_profile(count, total, reach, slope):
    weights = [(1 << 20) // math.isqrt(standing ** slope) + 1 for standing in range(2, count + 1)]
    spare, counts = total - reach - (count - 1), [1] * (count - 1)
    while spare > 0:
        movable = [i for i in range(count - 1) if counts[i] < reach]
        mass, budget = sum([weights[i] for i in movable]), spare
        for i in movable:
            addition = min(reach - counts[i], max(1, budget * weights[i] // mass), spare)
            counts[i] = counts[i] + addition
            spare = spare - addition
    return np.array([reach] + counts)


def uneven_parts(key, amount, total, bound, slope):
    if amount == 2:
        one = jax.random.randint(key, (), max(1, total - bound), min(bound, total - 1) + 1)
        return jnp.stack([one, total - one])
    sizes = jnp.asarray(length_profile(amount, total, bound, slope), jnp.int32)
    pairs = (amount - 1) // 2
    giver, sink = sizes[1:1 + 2 * pairs:2], sizes[2:2 + 2 * pairs:2]
    slack = jnp.minimum(giver - 1, bound - sink)
    moved = jax.random.randint(jax.random.fold_in(key, 1), (pairs,), 0, 1 << 20) % (slack + 1)
    sizes = sizes.at[1:1 + 2 * pairs:2].set(giver - moved).at[2:2 + 2 * pairs:2].set(sink + moved)
    return sizes[jax.random.permutation(jax.random.fold_in(key, 2), amount)]


def noise(key, shape, deviation, limit, cuts=(), kind=jnp.bfloat16):
    result = deviation * jax.random.normal(key, shape, jnp.float32)
    if cuts:
        result = result * block_levels(key, shape, cuts, -0.22, 0.18)
    return jnp.clip(result, -limit, limit).astype(kind)


def setup_inputs(seed: int = 0) -> dict:
    streams_of = jax.random.split(jax.random.key(seed), 20)
    return {
        "tokens": draw_tokens(jax.random.fold_in(streams_of[19], 71), 0),
        "first_gain": jnp.clip(1.0 + 0.18 * jax.random.normal(streams_of[1], (WIDTH,), jnp.float32), 0.1, 1.9),
        "first_gate": noise(streams_of[2], (WIDTH, FFN_UNITS), WIDTH ** -0.5, 0.09375, ((0, 8), (1, 4))),
        "first_up": noise(streams_of[3], (WIDTH, FFN_UNITS), WIDTH ** -0.5, 0.09375, ((0, 8), (1, 4))),
        "first_down": noise(streams_of[4], (FFN_UNITS, WIDTH), FFN_UNITS ** -0.5, 0.0546875, ((0, 4), (1, 8))),
        "mixer_gain": jnp.clip(1.0 + 0.18 * jax.random.normal(streams_of[5], (WIDTH,), jnp.float32), 0.1, 1.9),
        "w_query": noise(streams_of[6], (WIDTH, HEADS * 2 * HEAD_DIM), WIDTH ** -0.5, 0.09375, ((0, 8), (1, 4))),
        "w_key": noise(streams_of[7], (WIDTH, HEADS * 2 * HEAD_DIM), (3.5 / WIDTH ** 0.5), 0.328125, ((0, 8), (1, 4))),
        "w_value": noise(streams_of[8], (WIDTH, HEADS * VAL_DIM), WIDTH ** -0.5, 0.09375, ((0, 8), (1, 4))),
        "w_output": noise(streams_of[9], (HEADS * VAL_DIM, WIDTH), (HEADS * VAL_DIM) ** -0.5, 0.09375, ((0, 4), (1, 8))),
        "lam_heads": jnp.clip(0.3 + 0.5 * jax.random.uniform(streams_of[10], (HEADS,), jnp.float32) ** block_levels(streams_of[10], (HEADS,), ((0, 4),), -0.2, 0.2), 0.3, 0.8),
        "head_gain": jnp.clip(1.0 + 0.18 * jax.random.normal(streams_of[11], (VAL_DIM,), jnp.float32), 0.1, 1.9),
        "key_cache": draw_key_cache(jax.random.fold_in(streams_of[19], 71), 0),
        "value_cache": noise(streams_of[13], (BATCH, SEQ_LEN, HEADS, VAL_DIM), 1.0, 6.0, ((1, 8), (2, 4))),
        "lengths": uneven_parts(streams_of[14], BATCH, 3 * SEQ_LEN * BATCH // 8, SEQ_LEN, 2).astype(jnp.int32),
        "last_gain": jnp.clip(1.0 + 0.18 * jax.random.normal(streams_of[15], (WIDTH,), jnp.float32), 0.1, 1.9),
        "last_gate": noise(streams_of[16], (WIDTH, FFN_UNITS), WIDTH ** -0.5, 0.09375, ((0, 8), (1, 4))),
        "last_up": noise(streams_of[17], (WIDTH, FFN_UNITS), WIDTH ** -0.5, 0.09375, ((0, 8), (1, 4))),
        "last_down": noise(streams_of[18], (FFN_UNITS, WIDTH), FFN_UNITS ** -0.5, 0.0546875, ((0, 4), (1, 8))),
    }


epsilon = 1e-06
neg_fill = -1e+30

def gated_units(stream, gain, gate_w, up_w, down_w):
    wide = stream.astype(jnp.float32)
    inv_rms = lax.rsqrt(lax.optimization_barrier(jnp.mean(wide * wide, axis=1, keepdims=True)) + epsilon)
    scaled = (wide * gain).astype(jnp.bfloat16)
    gate_pre = jnp.dot(scaled, gate_w, preferred_element_type=jnp.float32) * inv_rms
    up_pre = jnp.dot(scaled, up_w, preferred_element_type=jnp.float32) * inv_rms
    hidden_act = (jax.nn.silu(gate_pre) * up_pre).astype(jnp.bfloat16)
    return jnp.dot(hidden_act, down_w, preferred_element_type=jnp.float32)

def one_sequence(items):
    query_rows, keys, values, length, fresh_key, new_value, lam_heads = items
    seq_len = keys.shape[0]
    logit_scale = HEAD_DIM ** (-0.5)
    query_single32 = query_rows.astype(jnp.float32)
    key_entries = keys.astype(jnp.float32).reshape(seq_len, HEADS, 2, HEAD_DIM)
    score_matrix = jnp.einsum('fuz,tfuz->fut', query_single32, key_entries) * logit_scale
    positions = jnp.arange(seq_len, dtype=jnp.int32)
    live_mask = (positions < length)[None, None, :]
    score_matrix = jnp.where(live_mask, score_matrix, neg_fill)
    self_score = jnp.einsum('vij,vij->vi', query_single32, fresh_key.astype(jnp.float32)) * logit_scale
    highest = jnp.maximum(lax.optimization_barrier(jnp.max(score_matrix, axis=-1)), self_score)
    weights = jnp.where(live_mask, jnp.exp(score_matrix - highest[..., None]), 0.0)
    own_weight = jnp.exp(self_score - highest)
    totals = lax.optimization_barrier(jnp.sum(weights, axis=-1)) + own_weight
    rounded = lax.optimization_barrier(weights.astype(jnp.bfloat16)).astype(jnp.float32)
    own_round = lax.optimization_barrier(own_weight.astype(jnp.bfloat16)).astype(jnp.float32)
    weighted = jnp.einsum('hml,lhe->hme', rounded, values.astype(jnp.float32))
    weighted = weighted + own_round[..., None] * new_value.astype(jnp.float32)[:, None, :]
    return weighted[:, 0] / totals[:, 0, None] - lam_heads[:, None] * weighted[:, 1] / totals[:, 1, None]

def reference(tokens, first_gain, first_gate, first_up, first_down, mixer_gain, w_query, w_key, w_value, w_output, lam_heads, head_gain, key_cache, value_cache, lengths, last_gain, last_gate, last_up, last_down):
    batch = tokens.shape[0]
    first = (tokens.astype(jnp.float32) + 0.5 * gated_units(tokens, first_gain, first_gate, first_up, first_down)).astype(jnp.bfloat16)
    wide = first.astype(jnp.float32)
    inv_rms = lax.rsqrt(lax.optimization_barrier(jnp.mean(wide * wide, axis=1, keepdims=True)) + epsilon)
    scaled = (wide * mixer_gain).astype(jnp.bfloat16)
    query_rows = (jnp.dot(scaled, w_query, preferred_element_type=jnp.float32) * inv_rms).astype(jnp.bfloat16)
    fresh_key = (jnp.dot(scaled, w_key, preferred_element_type=jnp.float32) * inv_rms).astype(jnp.bfloat16)
    new_value = (jnp.dot(scaled, w_value, preferred_element_type=jnp.float32) * inv_rms).astype(jnp.bfloat16)
    query_rows = query_rows.reshape(batch, HEADS, 2, HEAD_DIM)
    fresh_key = fresh_key.reshape(batch, HEADS, 2, HEAD_DIM)
    new_value = new_value.reshape(batch, HEADS, VAL_DIM)
    lam_rows = jnp.broadcast_to(lam_heads, (batch, HEADS))
    mixed = lax.map(one_sequence, (query_rows, key_cache, value_cache, lengths, fresh_key, new_value, lam_rows))
    normed = mixed * lax.rsqrt(lax.optimization_barrier(jnp.mean(mixed * mixed, axis=-1, keepdims=True)) + epsilon) * head_gain
    attended = normed.astype(jnp.bfloat16).reshape(batch, HEADS * VAL_DIM)
    projected = jnp.dot(attended, w_output, preferred_element_type=jnp.float32)
    second = (wide + projected).astype(jnp.bfloat16)
    last = gated_units(second, last_gain, last_gate, last_up, last_down)
    return (second.astype(jnp.float32) + 0.5 * last).astype(jnp.bfloat16)
```

```python
import functools

import jax
import jax.numpy as jnp
from jax import lax
from jax.experimental import pallas as pl
from jax.experimental.pallas import tpu as pltpu
from jax.sharding import PartitionSpec as P

HEAD_DIM = 64
VAL_DIM = 128
LANE = 128
epsilon = 1e-06
neg_fill = -1e30
bf16 = jnp.bfloat16
f32 = jnp.float32
MESH = pl.DeviceIdType.MESH


def ceil_div(a, b):
    return -(-a // b)


def layer_kernel(cfg, names, *refs):
    r = dict(zip(names, refs))
    n, t, rows = cfg["n"], cfg["t"], cfg["rows"]
    heads, positions = cfg["heads"], cfg["positions"]
    base, rem, lo, tiles = cfg["base"], cfg["rem"], cfg["lo"], cfg["tiles"]
    owners, per, first_owner = cfg["owners"], cfg["per"], cfg["first_owner"]
    cols, gather_here = cfg["cols"], cfg["gather_here"]
    chunks, chunk = cfg["chunks"], cfg["chunk"]
    units = cfg["units"]
    inner = heads * VAL_DIM
    share = per * VAL_DIM
    main = base * LANE
    me_k = lax.axis_index("kv")
    me_t = lax.axis_index("tp")
    halved = n & (n - 1) == 0

    load_count = [0]

    def load(source, target):
        load_count[0] += 1
        return pltpu.make_async_copy(source, target, r["load_sem"].at[load_count[0] - 1])

    def padded(ref, axis, size):
        if ref.shape[axis] == size:
            return ref
        return ref.at[:, pl.ds(0, size)] if axis == 1 else ref.at[pl.ds(0, size)]

    loads = {
        "tokens": load(r["tokens"], r["tok_all"].at[me_t] if gather_here else r["tok_in"]),
        "gain0": load(r["gain0_in"], r["gain0"]),
        "gain1": load(r["gain1_in"], r["gain1"]),
        "gain2": load(r["gain2_in"], r["gain2"]),
        "head_gain": load(r["head_gain_in"], r["head_gain"]),
        "lam": load(r["lam_in"], r["lam"]),
        "lengths": load(r["lengths_in"], r["lengths"]),
        "g1": load(r["first_gate"], padded(r["g1"], 1, units)),
        "u1": load(r["first_up"], padded(r["u1"], 1, units)),
        "d1": load(r["first_down"], padded(r["d1"], 0, units)),
        "wq": load(r["w_query"], r["wq"]),
        "wk": load(r["w_key"], r["wk"]),
        "wv": load(r["w_value"], r["wv"]),
        "kc": load(r["keys"], r["kc"]),
        "vc": load(r["values"], r["vc"]),
        "wo": load(r["w_output"], r["wo"]),
        "g2": load(r["last_gate"], padded(r["g2"], 1, units)),
        "u2": load(r["last_up"], padded(r["u2"], 1, units)),
        "d2": load(r["last_down"], padded(r["d2"], 0, units)),
    }

    def begin(*which):
        for name in which:
            loads[name].start()

    def finish(*which):
        for name in which:
            loads[name].wait()

    small = ("gain0", "gain1", "gain2", "head_gain", "lam", "lengths")
    begin("tokens", "g1", "u1", *small, "kc")

    barrier = pltpu.get_barrier_semaphore()
    for i in range(1, n):
        pl.semaphore_signal(
            barrier, inc=1, device_id=(lax.rem(me_k + i, n), me_t), device_id_type=MESH
        )
    for i in range(1, t):
        pl.semaphore_signal(
            barrier, inc=1, device_id=(me_k, lax.rem(me_t + i, t)), device_id_type=MESH
        )

    for name in ("g1", "u1", "g2", "u2"):
        ref = r[name]
        if ref.shape[1] > units:
            ref[:, units:] = jnp.zeros((ref.shape[0], ref.shape[1] - units), bf16)
    for name in ("d1", "d2"):
        ref = r[name]
        if ref.shape[0] > units:
            ref[units:, :] = jnp.zeros((ref.shape[0] - units, ref.shape[1]), bf16)

    flat = positions * heads
    row_head = lax.rem(lax.broadcasted_iota(jnp.int32, (2 * heads, flat), 0), heads)
    column = lax.broadcasted_iota(jnp.int32, (2 * heads, flat), 1)
    r["pos"][...] = jnp.where(
        lax.rem(column, heads) == row_head,
        column // heads + me_k * positions,
        jnp.int32(2**30),
    )
    pick_row = lax.broadcasted_iota(jnp.int32, (LANE, 4 * LANE), 0)
    pick_block = lax.broadcasted_iota(jnp.int32, (LANE, 4 * LANE), 1) // LANE
    r["pick"][...] = jnp.where(pick_row // 3 == pick_block, 1.0, 0.0).astype(bf16)

    finish("tokens")
    pl.semaphore_wait(barrier, n + t - 2)

    def partner(me, size, step):
        if size & (size - 1):
            return lax.rem(me + step, size)
        other, bit = 0, 1
        while bit < size:
            digit = lax.rem(me // bit, 2)
            other = other + bit * (1 - digit if step & bit else digit)
            bit *= 2
        return other

    far_first = list(range(n - 1, 0, -1))
    near_first = list(range(1, n))
    kv_partner = [partner(me_k, n, i) if i else me_k for i in range(n)]
    tp_partner = [partner(me_t, t, i) if i else me_t for i in range(t)]
    kv_source = kv_partner if halved else [lax.rem(me_k + n - i, n) for i in range(n)]
    sends = []

    def device(index, axis):
        return (index, me_t) if axis == "kv" else (me_k, index)

    def when(condition, action):
        if condition is None:
            action()
        else:
            pl.when(condition)(action)

    def ship(source, target, sem, index, axis, condition=None):
        copy = pltpu.make_async_remote_copy(
            src_ref=source,
            dst_ref=target,
            send_sem=r["send_sem"].at[len(sends)],
            recv_sem=sem,
            device_id=device(index, axis),
            device_id_type=MESH,
        )
        when(condition, copy.start)
        sends.append((copy, condition))

    def arrive(ref, sem):
        pltpu.make_async_remote_copy(
            src_ref=ref,
            dst_ref=ref,
            send_sem=r["send_sem"].at[0],
            recv_sem=sem,
            device_id=(me_k, me_t),
            device_id_type=MESH,
        ).wait_recv()

    def tp_broadcast(buffer, sems):
        for peer in tp_partner[:0:-1]:
            ship(buffer.at[me_t], buffer.at[me_t], sems.at[me_t], peer, "tp")

    def tp_await(buffer, sems):
        for i in range(1, t):
            source = lax.rem(me_t + t - i, t)
            arrive(buffer.at[source], sems.at[source])

    def dot(a, b):
        return jnp.dot(a, b, preferred_element_type=f32)

    def lanes(start, size):
        return pl.ds(pl.multiple_of(start, LANE), size)

    lane = lax.broadcasted_iota(jnp.int32, (rows, LANE), 1)
    diagonal = lane == lax.broadcasted_iota(jnp.int32, (rows, LANE), 0)

    def send_squares(wide, which):
        squares = jnp.sum(wide * wide, axis=1, keepdims=True)
        buffer, sems = r["squares"].at[which], r["sq_sem"].at[which]
        buffer[me_k] = jnp.sum(jnp.where(diagonal, squares, 0.0), axis=0, keepdims=True)
        for i in far_first:
            ship(buffer.at[me_k], buffer.at[me_k], sems.at[me_k], kv_partner[i], "kv")

    def inverse(which):
        buffer, sems = r["squares"].at[which], r["sq_sem"].at[which]
        for i in near_first:
            arrive(buffer.at[kv_source[i]], sems.at[kv_source[i]])
        total = buffer[0]
        for source in range(1, n):
            total += buffer[source]
        column_sum = jnp.sum(jnp.where(diagonal, total, 0.0), axis=1, keepdims=True)
        return lax.rsqrt(column_sum / cfg["model"] + epsilon)

    def scaled_by(wide, which):
        return (wide * r[f"gain{which}"][...]).astype(bf16)

    def start(owner):
        return owner * base + jnp.clip(owner - lo, 0, rem)

    def extra(owner):
        return jnp.logical_and(owner >= lo, owner < lo + rem)

    def gated(wide, which, gate, up, down, down_name, send, recv, sems, hid, hid_sems, fill):
        send_squares(wide, which)
        scaled = scaled_by(wide, which)
        order = far_first + [0]

        def part(owner, offset, size):
            place = lanes((start(owner) + offset) * LANE, size)
            return dot(scaled, gate[:, place]).astype(bf16), dot(scaled, up[:, place]).astype(bf16)

        if base:
            for i in order:
                owner = kv_partner[i]
                target = send.at[owner] if i else recv.at[me_k]
                g, u = part(owner, 0, main)
                target[:, :main] = g
                target[:, main : 2 * main] = u
                if i:
                    cut = pl.ds(0, 2 * main)
                    ship(
                        send.at[owner, :, cut],
                        recv.at[me_k, :, cut],
                        sems.at[0, me_k],
                        owner,
                        "kv",
                    )
        if rem:
            for i in order:
                owner = kv_partner[i]
                target = send.at[owner] if i else recv.at[me_k]
                g, u = part(owner, base, LANE)
                target[:, 2 * main : 2 * main + LANE] = g
                target[:, 2 * main + LANE :] = u
                if i:
                    cut = pl.ds(2 * main, 2 * LANE)
                    ship(
                        send.at[owner, :, cut],
                        recv.at[me_k, :, cut],
                        sems.at[1, me_k],
                        owner,
                        "kv",
                        extra(owner),
                    )
        fill()
        inv = inverse(which)

        def activate(index, begin_at, size):
            cut = slice(begin_at, begin_at + 2 * size)
            total = recv[me_k, :, cut].astype(f32)
            for i in near_first:
                source = kv_source[i]
                arrive(recv.at[source, :, pl.ds(begin_at, 2 * size)], sems.at[index, source])
                total += recv[source, :, cut].astype(f32)
            a = total[:, :size] * inv
            b = total[:, size:] * inv
            return (a * (1.0 / (1.0 + jnp.exp(-a))) * b).astype(bf16)

        my_main = lanes(start(me_k) * LANE, main) if base else None
        my_extra = lanes((start(me_k) + base) * LANE, LANE)
        mine = extra(me_k)
        if base:
            hid[:, my_main] = activate(0, 0, main)
            for i in far_first:
                ship(
                    hid.at[:, my_main],
                    hid.at[:, my_main],
                    hid_sems.at[0, me_k],
                    kv_partner[i],
                    "kv",
                )
        if rem:

            def do_extra():
                hid[:, my_extra] = activate(1, 2 * main, LANE)

            pl.when(mine)(do_extra)
            for i in far_first:
                ship(
                    hid.at[:, my_extra],
                    hid.at[:, my_extra],
                    hid_sems.at[1, me_k],
                    kv_partner[i],
                    "kv",
                    mine,
                )
        finish(down_name)

        def hid_arrive(indices):
            for i in indices:
                source = kv_source[i]
                if base:
                    place = lanes(start(source) * LANE, main)
                    arrive(hid.at[:, place], hid_sems.at[0, source])
            for i in indices:
                source = kv_source[i]
                if rem:
                    place = lanes((start(source) + base) * LANE, LANE)

                    def wait_extra():
                        arrive(hid.at[:, place], hid_sems.at[1, source])

                    pl.when(extra(source))(wait_extra)

        half_tiles = (n // 2) * base + min(max(n // 2 - lo, 0), rem)
        if halved and n > 1 and half_tiles * 2 == tiles:
            size = half_tiles * LANE
            near = jnp.where(me_k < n // 2, 0, size)
            hid_arrive(range(1, n // 2))
            total = dot(hid[:, lanes(near, size)], down[lanes(near, size), :])
            hid_arrive(range(n // 2, n))
            far = size - near
            return total + dot(hid[:, lanes(far, size)], down[lanes(far, size), :])
        hid_arrive(near_first)
        size = tiles * LANE
        return dot(hid[:, :size], down[...])

    def tp_total(part, buffer, sems):
        buffer[me_t] = part.astype(bf16)
        tp_broadcast(buffer, sems)
        tp_await(buffer, sems)
        total = buffer[0].astype(f32)
        for source in range(1, t):
            total += buffer[source].astype(f32)
        return total

    if gather_here:
        tok_all = r["tok_all"]
        for i in range(t - 1, 0, -1):
            ship(tok_all.at[me_t], tok_all.at[me_t], r["tok_sem"].at[me_t], tp_partner[i], "tp")
    begin("d1", "wq", "wk", "wv", "vc", "wo", "g2", "u2", "d2")
    finish("g1", "u1", *small)
    if gather_here:
        tp_await(tok_all, r["tok_sem"])
        wide = jnp.concatenate([tok_all[s].astype(f32) for s in range(t)], axis=1)
    else:
        wide = r["tok_in"][...].astype(f32)

    def nothing():
        pass

    def turn_keys(lower, upper):
        kc, kt = r["kc"], r["kt"]

        def one(b, carry):
            kt[b] = kc[b].T
            return carry

        lax.fori_loop(lower, upper, one, 0, unroll=2)

    def first_fill():
        if cfg["turned"]:
            finish("kc")
            turn_keys(0, rows)

    part = gated(
        wide,
        0,
        r["g1"],
        r["u1"],
        r["d1"],
        "d1",
        r["gu_send1"],
        r["gu_recv1"],
        r["gu_sem1"],
        r["hid1"],
        r["hid_sem1"],
        first_fill,
    )
    first = (wide + 0.5 * tp_total(part, r["down1"], r["down_sem1"])).astype(bf16).astype(f32)

    finish("wq")
    send_squares(first, 1)
    scaled = scaled_by(first, 1)
    query_part = dot(scaled, r["wq"][...]).astype(bf16)
    q_send, q_recv, q_sem = r["q_send"], r["q_recv"], r["q_sem"]
    for c in range(chunks):
        q_send[c] = query_part[c * chunk : (c + 1) * chunk]
    for c in range(chunks):
        for i in far_first:
            ship(q_send.at[c], q_recv.at[me_k, c], q_sem.at[me_k, c], kv_partner[i], "kv")

    kv_send, kv_recv, kv_sem = r["kv_send"], r["kv_recv"], r["kv_sem"]
    finish("wk", "wv")
    key_part = dot(scaled, r["wk"][...]).astype(bf16)
    value_part = dot(scaled, r["wv"][...]).astype(bf16)
    shift = jnp.where(me_k < n // 2, owners // 2, 0)
    my_place = me_k - first_owner
    is_owner = jnp.logical_and(my_place >= 0, my_place < owners)
    my_slot = jnp.clip(my_place, 0, owners - 1)
    for j in range(owners):
        kv_send[j, :, :share] = key_part[:, j * share : (j + 1) * share]
        kv_send[j, :, share:] = value_part[:, j * share : (j + 1) * share]
    owner_order = [lax.rem(j + shift, owners) for j in range(owners)]
    for j in owner_order:
        owner = j + first_owner
        ship(kv_send.at[j], kv_recv.at[me_k], kv_sem.at[me_k], owner, "kv", me_k != owner)

    inv = inverse(1)
    logit_scale = HEAD_DIM ** (-0.5)
    wide_lane = lax.broadcasted_iota(jnp.int32, (2 * heads, LANE), 1)
    third = lax.rem(wide_lane, 3)
    map_row = lax.broadcasted_iota(jnp.int32, (2 * heads, LANE), 0) // heads
    slot = wide_lane - 6 * map_row
    first_half = lax.broadcasted_iota(jnp.int32, (chunk, LANE), 1) < HEAD_DIM
    finish("vc")
    if not cfg["turned"]:
        finish("kc")
    kc, vc, kt, qf, acc, q_all = r["kc"], r["vc"], r["kt"], r["qf"], r["acc"], r["q_all"]
    score_ref, pos, lengths = r["score"], r["pos"], r["lengths"]
    att_send, att_recv, part_sem = r["att_send"], r["att_recv"], r["part_sem"]

    def attend(c):
        total = q_send[c].astype(f32)
        for i in near_first:
            source = kv_source[i]
            arrive(q_recv.at[source, c], q_sem.at[source, c])
            total += q_recv[source, c].astype(f32)
        query = (total * inv[c * chunk : (c + 1) * chunk]).astype(bf16)
        q_all[c * chunk : (c + 1) * chunk, :] = query.astype(f32)
        for h in range(heads):
            block = query[:, h * VAL_DIM : (h + 1) * VAL_DIM].astype(f32) * logit_scale
            qf[:, h, :] = jnp.where(first_half, block, 0.0)
            qf[:, heads + h, :] = jnp.where(first_half, 0.0, block)
        for i in range(chunk):
            b = c * chunk + i
            if cfg["turned"]:
                score_ref[i] = dot(qf[i].astype(bf16), kt[b])
            else:
                score_ref[i] = lax.dot_general(
                    qf[i].astype(bf16),
                    kc[b],
                    (((1,), (1,)), ((), ())),
                    preferred_element_type=f32,
                )
        for i in range(chunk):
            b = c * chunk + i
            score = jnp.where(pos[...] < lengths[b], score_ref[i], neg_fill)
            peak = jnp.max(score, axis=1, keepdims=True)
            weight = jnp.exp(score - peak)
            mass = jnp.sum(weight, axis=1, keepdims=True)
            acc[i, :, :LANE] = dot(weight.astype(bf16), vc[b])
            stats = jnp.where(
                slot < 0, 0.0, jnp.where(slot < 3, peak, jnp.where(slot < 6, mass, 0.0))
            )
            high = stats.astype(bf16).astype(f32)
            mid = (stats - high).astype(bf16).astype(f32)
            low = stats - high - mid
            acc[i, :, LANE:] = jnp.where(third == 0, high, jnp.where(third == 1, mid, low))
        for j in range(owners):
            for p in range(per):
                head = j * per + p
                one, two = acc[:, head, :], acc[:, heads + head, :]
                place = pl.ds(p * chunk, chunk)
                att_send[c, j, place, :LANE] = one[:, :LANE].astype(bf16)
                att_send[c, j, place, LANE : 2 * LANE] = two[:, :LANE].astype(bf16)
                att_send[c, j, place, 2 * LANE :] = (one[:, LANE:] + two[:, LANE:]).astype(bf16)
        for j in owner_order:
            owner = j + first_owner
            ship(
                att_send.at[c, j],
                att_recv.at[me_k, c],
                part_sem.at[me_k, c],
                owner,
                "kv",
                me_k != owner,
            )

    for c in range(chunks):
        attend(c)

    att_all, att_sem = r["att_all"], r["att_sem"]
    my_share = lanes(my_slot * share, share)
    half = lax.broadcasted_iota(jnp.int32, (per * chunk, LANE), 1) < HEAD_DIM

    def combine():
        kv_recv[me_k] = kv_send[my_slot]
        for i in near_first:
            source = kv_source[i]
            arrive(kv_recv.at[source], kv_sem.at[source])
        fresh = kv_recv[0].astype(f32)
        for source in range(1, n):
            fresh += kv_recv[source].astype(f32)
        fresh = (fresh * inv).astype(bf16).astype(f32)
        fresh_key, fresh_value = fresh[:, :share], fresh[:, share:]
        query = q_all[:, my_share]
        product = query * fresh_key * logit_scale

        def stacked(x, c):
            return jnp.concatenate(
                [
                    x[c * chunk : (c + 1) * chunk, p * VAL_DIM : (p + 1) * VAL_DIM]
                    for p in range(per)
                ],
                axis=0,
            )

        own = []
        for c in range(chunks):
            block = stacked(product, c)
            own.append(
                [
                    jnp.sum(jnp.where(half, block, 0.0), axis=1, keepdims=True),
                    jnp.sum(jnp.where(half, 0.0, block), axis=1, keepdims=True),
                ]
            )
        lam_rows = jnp.concatenate(
            [jnp.full((chunk, LANE), r["lam"][my_slot * per + p], f32) for p in range(per)], axis=0
        )
        for c in range(chunks):
            att_recv[me_k, c] = att_send[c, my_slot]
            for i in near_first:
                source = kv_source[i]
                arrive(att_recv.at[source, c], part_sem.at[source, c])
            stats = jnp.concatenate(
                [att_recv[source, c, :, 2 * LANE :] for source in range(n)], axis=0
            )
            stats = dot(stats, r["pick"][...])
            high = per * chunk
            new_value = stacked(fresh_value, c)
            maps = []
            for m in range(2):
                peaks = [
                    stats[s * high : (s + 1) * high, 2 * m * LANE : (2 * m + 1) * LANE]
                    for s in range(n)
                ]
                masses = [
                    stats[s * high : (s + 1) * high, (2 * m + 1) * LANE : (2 * m + 2) * LANE]
                    for s in range(n)
                ]
                highest = jnp.broadcast_to(own[c][m], (high, LANE))
                for peak in peaks:
                    highest = jnp.maximum(highest, peak)
                own_weight = jnp.exp(own[c][m] - highest)
                den = own_weight
                num = own_weight.astype(bf16).astype(f32) * new_value
                for source in range(n):
                    scale = jnp.exp(peaks[source] - highest)
                    den += scale * masses[source]
                    num += scale * att_recv[source, c, :, m * LANE : (m + 1) * LANE].astype(f32)
                maps.append(num / den)
            mixed = maps[0] - lam_rows * maps[1]
            normed = (
                mixed
                * lax.rsqrt(jnp.mean(mixed * mixed, axis=1, keepdims=True) + epsilon)
                * r["head_gain"][...]
            )
            for p in range(per):
                r["att_own"][c * chunk : (c + 1) * chunk, p * VAL_DIM : (p + 1) * VAL_DIM] = (
                    normed[p * chunk : (p + 1) * chunk]
                )
        att_all[:, my_share] = r["att_own"][...].astype(bf16)

    pl.when(is_owner)(combine)
    for i in far_first:
        ship(
            att_all.at[:, my_share],
            att_all.at[:, my_share],
            att_sem.at[my_slot],
            kv_partner[i],
            "kv",
            is_owner,
        )
    finish("wo")

    def att_arrive(j):
        place = lanes(j * share, share)

        def wait_share():
            arrive(att_all.at[:, place], att_sem.at[j])

        pl.when(me_k != j + first_owner)(wait_share)

    wo = r["wo"]
    if halved and owners % 2 == 0 and 2 * first_owner + owners == n:
        size = owners // 2 * share
        near_low = me_k < n // 2
        near_slot = jnp.where(near_low, 0, owners // 2)
        far_slot = owners // 2 - near_slot
        for j in range(owners // 2):
            att_arrive(near_slot + j)
        near = near_slot * share
        part = dot(att_all[:, lanes(near, size)], wo[lanes(near, size), :])
        for j in range(owners // 2):
            att_arrive(far_slot + j)
        far = far_slot * share
        part += dot(att_all[:, lanes(far, size)], wo[lanes(far, size), :])
    else:
        for j in range(owners):
            att_arrive(jnp.int32(j))
        part = dot(att_all[...], wo[...])
    second = (first + tp_total(part, r["out_all"], r["out_sem"])).astype(bf16).astype(f32)

    finish("g2", "u2")
    stream, result = r["stream"], r["result"]
    stream[...] = second
    part = gated(
        second,
        2,
        r["g2"],
        r["u2"],
        r["d2"],
        "d2",
        r["gu_send2"],
        r["gu_recv2"],
        r["gu_sem2"],
        r["hid2"],
        r["hid_sem2"],
        nothing,
    )
    if gather_here:
        down2, down2_recv, sems = r["down2"], r["down2_recv"], r["down_sem2"]
        for s in range(t):
            down2[s] = part[:, s * cols : (s + 1) * cols]
        for peer in tp_partner[:0:-1]:
            ship(down2.at[peer], down2_recv.at[me_t], sems.at[me_t], peer, "tp")
        down2_recv[me_t] = down2[me_t]
        tp_await(down2_recv, sems)
        total = down2_recv[0]
        for source in range(1, t):
            total += down2_recv[source]
        own = stream[:, lanes(me_t * cols, cols)]
        result[...] = (own + 0.5 * total).astype(bf16)
    else:
        total = tp_total(part, r["down2"], r["down_sem2"])
        result[...] = (second + 0.5 * total).astype(bf16)
    for copy, condition in sends:
        when(condition, copy.wait_send)


def on_device(
    tokens,
    first_gain,
    first_gate,
    first_up,
    first_down,
    mixer_gain,
    w_query,
    w_key,
    w_value,
    w_output,
    lam_heads,
    head_gain,
    key_cache,
    value_cache,
    lengths,
    last_gain,
    last_gate,
    last_up,
    last_down,
):
    n, t = lax.axis_size("kv"), lax.axis_size("tp")
    rows, cols = tokens.shape
    width, units = first_gate.shape
    positions, heads = key_cache.shape[1:3]
    gather_here = cols % LANE == 0
    tiles = ceil_div(units, LANE)
    base, rem = divmod(tiles, n)
    lo = (n - rem) // 2
    owners = heads // 2 if heads % 2 == 0 and heads // 2 <= n else heads
    per = heads // owners
    chunks = 2 if rows % 16 == 0 else 1
    chunk = rows // chunks
    inner = heads * VAL_DIM
    share = per * VAL_DIM
    cfg = dict(
        n=n,
        t=t,
        model=width * n,
        rows=rows,
        cols=cols,
        units=units,
        heads=heads,
        positions=positions,
        tiles=tiles,
        base=base,
        rem=rem,
        lo=lo,
        owners=owners,
        per=per,
        first_owner=(n - owners) // 2,
        gather_here=gather_here,
        chunks=chunks,
        chunk=chunk,
        turned=TURNED,
    )
    if not gather_here:
        tokens = lax.all_gather(tokens, "tp", axis=1, tiled=True)
    flat = positions * heads
    keys = key_cache.reshape(rows, flat, VAL_DIM)
    values = value_cache.reshape(rows, flat, VAL_DIM)

    wide_units = (tiles + (1 if rem else 0)) * LANE
    gu = (n, rows, 2 * (base + (1 if rem else 0)) * LANE)
    dma = pltpu.SemaphoreType.DMA
    return_cols = cols if gather_here else width
    inputs = dict(
        tokens=tokens,
        gain0_in=first_gain.reshape(1, width),
        gain1_in=mixer_gain.reshape(1, width),
        gain2_in=last_gain.reshape(1, width),
        head_gain_in=head_gain.reshape(1, VAL_DIM),
        lam_in=lam_heads,
        lengths_in=lengths,
        first_gate=first_gate,
        first_up=first_up,
        first_down=first_down,
        w_query=w_query,
        w_key=w_key,
        w_value=w_value,
        w_output=w_output,
        keys=keys,
        values=values,
        last_gate=last_gate,
        last_up=last_up,
        last_down=last_down,
    )
    scratch = dict(
        gain0=((1, width), f32),
        gain1=((1, width), f32),
        gain2=((1, width), f32),
        head_gain=((1, VAL_DIM), f32),
        g1=((width, wide_units), bf16),
        u1=((width, wide_units), bf16),
        d1=((tiles * LANE, width), bf16),
        wq=((width, inner), bf16),
        wk=((width, inner), bf16),
        wv=((width, inner), bf16),
        wo=((inner, width), bf16),
        kc=((rows, flat, VAL_DIM), bf16),
        vc=((rows, flat, VAL_DIM), bf16),
        kt=((rows, VAL_DIM, flat) if TURNED else (1, VAL_DIM, LANE), bf16),
        g2=((width, wide_units), bf16),
        u2=((width, wide_units), bf16),
        d2=((tiles * LANE, width), bf16),
        stream=((rows, width), f32),
        squares=((3, n, 1, LANE), f32),
        gu_send1=(gu, bf16),
        gu_recv1=(gu, bf16),
        gu_send2=(gu, bf16),
        gu_recv2=(gu, bf16),
        hid1=((rows, wide_units), bf16),
        hid2=((rows, wide_units), bf16),
        down1=((t, rows, width), bf16),
        out_all=((t, rows, width), bf16),
        q_send=((chunks, chunk, inner), bf16),
        q_recv=((n, chunks, chunk, inner), bf16),
        q_all=((rows, inner), f32),
        kv_send=((owners, rows, 2 * share), bf16),
        kv_recv=((n, rows, 2 * share), bf16),
        qf=((chunk, 2 * heads, VAL_DIM), f32),
        score=((chunk, 2 * heads, flat), f32),
        acc=((chunk, 2 * heads, VAL_DIM + LANE), f32),
        pos=((2 * heads, flat), jnp.int32),
        pick=((LANE, 4 * LANE), bf16),
        att_send=((chunks, owners, per * chunk, 2 * VAL_DIM + LANE), bf16),
        att_recv=((n, chunks, per * chunk, 2 * VAL_DIM + LANE), bf16),
        att_own=((rows, share), f32),
        att_all=((rows, inner), bf16),
    )
    if gather_here:
        scratch.update(
            tok_all=((t, rows, cols), bf16),
            down2=((t, rows, cols), f32),
            down2_recv=((t, rows, cols), f32),
        )
    else:
        scratch.update(tok_in=((rows, width), bf16), down2=((t, rows, width), bf16))
    sends = (n - 1) * (3 + 8 + chunks + 1) + owners * (1 + chunks) + 4 * (t - 1)
    sems = dict(
        load_sem=(19,),
        send_sem=(sends,),
        tok_sem=(t,),
        sq_sem=(3, n),
        gu_sem1=(2, n),
        gu_sem2=(2, n),
        hid_sem1=(2, n),
        hid_sem2=(2, n),
        down_sem1=(t,),
        down_sem2=(t,),
        out_sem=(t,),
        q_sem=(n, chunks),
        kv_sem=(n,),
        part_sem=(n, chunks),
        att_sem=(owners,),
    )
    smem = dict(lam=(lam_heads.shape, f32), lengths=(lengths.shape, jnp.int32))
    names = [*inputs, "result", *scratch, *smem, *sems]
    result = pl.pallas_call(
        functools.partial(layer_kernel, cfg, names),
        out_shape=pltpu.VMEM((rows, return_cols), bf16),
        in_specs=[pl.BlockSpec(memory_space=pl.ANY)] * len(inputs),
        out_specs=pl.BlockSpec(memory_space=pltpu.VMEM),
        scratch_shapes=[pltpu.VMEM(shape, kind) for shape, kind in scratch.values()]
        + [pltpu.SMEM(shape, kind) for shape, kind in smem.values()]
        + [dma(shape) for shape in sems.values()],
        compiler_params=pltpu.CompilerParams(
            collective_id=0, has_side_effects=True, vmem_limit_bytes=63 * 2**20
        ),
    )(*inputs.values())
    if not gather_here:
        result = lax.dynamic_slice_in_dim(result, lax.axis_index("tp") * cols, cols, 1)
    return result


TURNED = True


def solution(mesh):
    return jax.shard_map(
        on_device,
        mesh=mesh,
        in_specs=(
            P(None, ("kv", "tp")),
            P("kv"),
            P("kv", "tp"),
            P("kv", "tp"),
            P("tp", "kv"),
            P("kv"),
            P("kv", "tp"),
            P("kv", "tp"),
            P("kv", "tp"),
            P("tp", "kv"),
            P("tp"),
            P(),
            P(None, "kv", "tp", None),
            P(None, "kv", "tp", None),
            P(),
            P("kv"),
            P("kv", "tp"),
            P("kv", "tp"),
            P("tp", "kv"),
        ),
        out_specs=P(None, ("kv", "tp")),
        check_vma=False,
    )
```

```python
import functools
import types

import jax
import jax.numpy as jnp
from jax import lax
from jax.experimental import pallas as pl
from jax.experimental.pallas import tpu as pltpu
from jax.sharding import PartitionSpec as P

HEAD_DIM = 64
VAL_DIM = 128
LANE = 128
epsilon = 1e-06
neg_fill = -1e30
bf16 = jnp.bfloat16
f32 = jnp.float32
MESH = pl.DeviceIdType.MESH


def ceil_div(a, b):
    return -(-a // b)


def layer_kernel(cfg, names, *refs):
    r = types.SimpleNamespace(**dict(zip(names, refs)))
    n, t, rows = cfg.n, cfg.t, cfg.rows
    heads, positions = cfg.heads, cfg.positions
    base, rem, lo, tiles = cfg.base, cfg.rem, cfg.lo, cfg.tiles
    owners, per, first_owner = cfg.owners, cfg.per, cfg.first_owner
    cols, gather_here = cfg.cols, cfg.gather_here
    chunks, chunk = cfg.chunks, cfg.chunk
    units = cfg.units
    inner = heads * VAL_DIM
    share = per * VAL_DIM
    main = base * LANE
    me_k = lax.axis_index("kv")
    me_t = lax.axis_index("tp")
    halved = n & (n - 1) == 0

    load_count = [0]

    def load(source, target):
        load_count[0] += 1
        return pltpu.make_async_copy(source, target, r.load_sem.at[load_count[0] - 1])

    def padded(ref, axis, size):
        if ref.shape[axis] == size:
            return ref
        return ref.at[:, pl.ds(0, size)] if axis == 1 else ref.at[pl.ds(0, size)]

    loads = types.SimpleNamespace(
        tokens=load(r.tokens, r.tok_all.at[me_t] if gather_here else r.tok_in),
        gain0=load(r.gain0_in, r.gain0),
        gain1=load(r.gain1_in, r.gain1),
        gain2=load(r.gain2_in, r.gain2),
        head_gain=load(r.head_gain_in, r.head_gain),
        lam=load(r.lam_in, r.lam),
        lengths=load(r.lengths_in, r.lengths),
        g1=load(r.first_gate, padded(r.g1, 1, units)),
        u1=load(r.first_up, padded(r.u1, 1, units)),
        d1=load(r.first_down, padded(r.d1, 0, units)),
        wq=load(r.w_query, r.wq),
        wk=load(r.w_key, r.wk),
        wv=load(r.w_value, r.wv),
        kc=load(r.keys, r.kc),
        vc=load(r.values, r.vc),
        wo=load(r.w_output, r.wo),
        g2=load(r.last_gate, padded(r.g2, 1, units)),
        u2=load(r.last_up, padded(r.u2, 1, units)),
        d2=load(r.last_down, padded(r.d2, 0, units)),
    )

    def begin(*which):
        for copy in which:
            copy.start()

    def finish(*which):
        for copy in which:
            copy.wait()

    small = (loads.gain0, loads.gain1, loads.gain2, loads.head_gain, loads.lam, loads.lengths)
    begin(loads.tokens, loads.g1, loads.u1, *small, loads.kc)

    def when(condition, action):
        if condition is None:
            action()
        else:
            pl.when(condition)(action)

    staged = n % 2 == 0 and 2 < n <= 8
    level, side, levels = me_k // 2, lax.rem(me_k, 2), n // 2
    barrier = pltpu.get_barrier_semaphore()

    def greet(sem, ranks):
        for rank, condition in ranks:

            def signal():
                pl.semaphore_signal(sem, inc=1, device_id=(rank, me_t), device_id_type=MESH)

            when(condition, signal)

    def count(ranks):
        total = jnp.int32(0)
        for _, condition in ranks:
            total += 1 if condition is None else condition.astype(jnp.int32)
        return total

    def reach(step, flip):
        if step == 0:
            return [(level * 2 + 1 - side, None)]
        to_side = 1 - side if flip else side
        return [
            ((level - step) * 2 + to_side, level >= step),
            ((level + step) * 2 + to_side, level < levels - step),
        ]

    if staged:
        adjacent = reach(0, True) + reach(1, False)
        within = adjacent + reach(1, True) + (reach(2, False) if levels > 2 else [])
    else:
        adjacent = [(lax.rem(me_k + i, n), None) for i in range(1, n)]
    greet(barrier, adjacent)
    for i in range(1, t):
        pl.semaphore_signal(
            barrier, inc=1, device_id=(me_k, lax.rem(me_t + i, t)), device_id_type=MESH
        )

    finish(loads.tokens)
    pl.semaphore_wait(barrier, count(adjacent) + (t - 1))

    def partner(me, size, step):
        if size & (size - 1):
            return lax.rem(me + step, size)
        other, bit = 0, 1
        while bit < size:
            digit = lax.rem(me // bit, 2)
            other = other + bit * (1 - digit if step & bit else digit)
            bit *= 2
        return other

    far_first = list(range(n - 1, 0, -1))
    near_first = list(range(1, n))
    kv_partner = [partner(me_k, n, i) if i else me_k for i in range(n)]
    tp_partner = [partner(me_t, t, i) if i else me_t for i in range(t)]
    kv_source = kv_partner if halved else [lax.rem(me_k + n - i, n) for i in range(n)]
    sends = []
    groups = []

    def device(index, axis):
        return (index, me_t) if axis == "kv" else (me_k, index)

    def ship(copies, sem, axis, keep=None):
        own = r.send_sem.at[len(groups)]
        if keep is None:
            groups.append(len(copies))
        for source, target, index, condition in copies:
            copy = pltpu.make_async_remote_copy(
                src_ref=source,
                dst_ref=target,
                send_sem=own,
                recv_sem=sem,
                device_id=device(index, axis),
                device_id_type=MESH,
            )
            when(condition, copy.start)
        return own

    def sent(own, ref, condition=None):
        copy = pltpu.make_async_remote_copy(
            src_ref=ref,
            dst_ref=ref,
            send_sem=own,
            recv_sem=own,
            device_id=(me_k, me_t),
            device_id_type=MESH,
        )
        sends.append((copy, condition))

    def arrive(ref, sem):
        pltpu.make_async_remote_copy(
            src_ref=ref,
            dst_ref=ref,
            send_sem=sem,
            recv_sem=sem,
            device_id=(me_k, me_t),
            device_id_type=MESH,
        ).wait_recv()

    def kv_broadcast(ref, sem):
        return ship([(ref, ref, kv_partner[i], None) for i in far_first], sem, "kv")

    def tp_broadcast(buffer, sem):
        block = buffer.at[me_t]
        own = ship([(block, block, peer, None) for peer in tp_partner[:0:-1]], sem, "tp")
        sent(own, buffer.at[pl.ds(0, t - 1)])

    def tp_await(buffer, sem):
        arrive(buffer.at[pl.ds(0, t - 1)], sem)

    def dot(a, b):
        return jnp.dot(a, b, preferred_element_type=f32)

    def lanes(start, size):
        return pl.ds(pl.multiple_of(start, LANE), size)

    lane = lax.broadcasted_iota(jnp.int32, (rows, LANE), 1)
    diagonal = lane == lax.broadcasted_iota(jnp.int32, (rows, LANE), 0)

    def send_squares(wide, which):
        squares = jnp.sum(wide * wide, axis=1, keepdims=True)
        buffer, sems = r.squares.at[which], r.sq_sem.at[which]
        buffer[me_k] = jnp.sum(jnp.where(diagonal, squares, 0.0), axis=0, keepdims=True)
        own = kv_broadcast(buffer.at[me_k], sems)
        sent(own, buffer.at[pl.ds(0, n - 1)])

    def inverse(which):
        buffer, sems = r.squares.at[which], r.sq_sem.at[which]
        arrive(buffer.at[pl.ds(0, n - 1)], sems)
        total = buffer[0]
        for source in range(1, n):
            total += buffer[source]
        column_sum = jnp.sum(jnp.where(diagonal, total, 0.0), axis=1, keepdims=True)
        return lax.rsqrt(column_sum / cfg.model + epsilon)

    def scaled_by(wide, which):
        return (wide * (r.gain0, r.gain1, r.gain2)[which][...]).astype(bf16)

    def start(owner):
        return owner * base + jnp.clip(owner - lo, 0, rem)

    def extra(owner):
        return jnp.logical_and(owner >= lo, owner < lo + rem)

    def gated(wide, which, gate, up, down, down_load, send, recv, sems, hid, hid_sems, fill):
        scaled = scaled_by(wide, which)
        order = far_first + [0]

        def part(owner, offset, size):
            place = lanes((start(owner) + offset) * LANE, size)
            return dot(scaled, gate[:, place]).astype(bf16), dot(scaled, up[:, place]).astype(bf16)

        def scatter(index, offset, size, begin_at):
            cut = pl.ds(begin_at, 2 * size)
            own = None
            for i in order:
                owner = kv_partner[i]
                target = send.at[owner] if i else recv.at[me_k]
                g, u = part(owner, offset, size)
                target[:, begin_at : begin_at + size] = g
                target[:, begin_at + size : begin_at + 2 * size] = u
                if i:
                    copy = pltpu.make_async_remote_copy(
                        src_ref=send.at[owner, :, cut],
                        dst_ref=recv.at[me_k, :, cut],
                        send_sem=r.send_sem.at[len(groups)],
                        recv_sem=sems.at[index],
                        device_id=(owner, me_t),
                        device_id_type=MESH,
                    )
                    when(extra(owner) if index else None, copy.start)
            own = r.send_sem.at[len(groups)]
            groups.append(n - 1)
            if index == 0:
                sent(own, send.at[pl.ds(0, n - 1), :, cut])
            else:
                mine = extra(me_k)
                if rem > 1:
                    sent(own, send.at[pl.ds(0, rem - 1), :, cut], mine)
                sent(own, send.at[pl.ds(0, rem), :, cut], jnp.logical_not(mine))

        if base:
            scatter(0, 0, main, 0)
        send_squares(wide, which)
        if rem:
            scatter(1, base, LANE, 2 * main)
        fill()
        inv = inverse(which)

        def activate(index, begin_at, size):
            cut = slice(begin_at, begin_at + 2 * size)
            arrive(recv.at[pl.ds(0, n - 1), :, pl.ds(begin_at, 2 * size)], sems.at[index])
            total = recv[0, :, cut].astype(f32)
            for source in range(1, n):
                total += recv[source, :, cut].astype(f32)
            a = total[:, :size] * inv
            b = total[:, size:] * inv
            return (a * (1.0 / (1.0 + jnp.exp(-a))) * b).astype(bf16)

        my_main = lanes(start(me_k) * LANE, main) if base else None
        my_extra = lanes((start(me_k) + base) * LANE, LANE)
        mine = extra(me_k)
        half_tiles = (n // 2) * base + min(max(n // 2 - lo, 0), rem)
        halves = halved and n > 1 and half_tiles * 2 == tiles

        def hid_sem(i):
            return hid_sems.at[1 if halves and i >= n // 2 else 0]

        def hid_ship(place, size, condition):
            own = r.send_sem.at[len(groups)]
            groups.append(n - 1)
            for i in far_first:
                copy = pltpu.make_async_remote_copy(
                    src_ref=hid.at[:, place],
                    dst_ref=hid.at[:, place],
                    send_sem=own,
                    recv_sem=hid_sem(i),
                    device_id=(kv_partner[i], me_t),
                    device_id_type=MESH,
                )
                when(condition, copy.start)
            sent(own, send.at[pl.ds(0, n - 1), :, pl.ds(0, size)], condition)

        if base:
            hid[:, my_main] = activate(0, 0, main)
            hid_ship(my_main, main, None)
        if rem:

            def do_extra():
                hid[:, my_extra] = activate(1, 2 * main, LANE)

            pl.when(mine)(do_extra)
            hid_ship(my_extra, LANE, mine)
        finish(down_load)

        def hid_arrive(index, all_tiles, with_me):
            if not with_me:
                arrive(hid.at[:, pl.ds(0, all_tiles * LANE)], hid_sems.at[index])
                return

            def wait_for(count):
                def wait():
                    arrive(hid.at[:, pl.ds(0, count * LANE)], hid_sems.at[index])

                return wait

            if rem and all_tiles > base + 1:
                pl.when(mine)(wait_for(all_tiles - base - 1))
            if all_tiles > base:
                when(jnp.logical_not(mine) if rem else None, wait_for(all_tiles - base))

        if halves:
            size = half_tiles * LANE
            near = jnp.where(me_k < n // 2, 0, size)
            hid_arrive(0, half_tiles, True)
            total = dot(hid[:, lanes(near, size)], down[lanes(near, size), :])
            hid_arrive(1, half_tiles, False)
            far = size - near
            return total + dot(hid[:, lanes(far, size)], down[lanes(far, size), :])
        hid_arrive(0, tiles, True)
        size = tiles * LANE
        return dot(hid[:, :size], down[...])

    def tp_total(part, buffer, sems):
        buffer[me_t] = part.astype(bf16)
        tp_broadcast(buffer, sems)
        tp_await(buffer, sems)
        total = buffer[0].astype(f32)
        for source in range(1, t):
            total += buffer[source].astype(f32)
        return total

    if gather_here:
        tok_all = r.tok_all
        tp_broadcast(tok_all, r.tok_sem.at[0])
    if staged:
        greet(r.greet_sem.at[0], adjacent)
    begin(loads.d1, loads.wq, loads.wk, loads.wv, loads.vc, loads.wo, loads.g2, loads.u2, loads.d2)
    if staged:
        pl.semaphore_wait(r.greet_sem.at[0], count(adjacent))
        greet(r.greet_sem.at[1], within)
    for ref in (r.g1, r.u1):
        if ref.shape[1] > units:
            ref[:, units:] = jnp.zeros((ref.shape[0], ref.shape[1] - units), bf16)
    finish(loads.g1, loads.u1, *small)
    if staged:
        pl.semaphore_wait(r.greet_sem.at[1], count(within))
    if gather_here:
        tp_await(tok_all, r.tok_sem.at[0])
        wide = jnp.concatenate([tok_all[s].astype(f32) for s in range(t)], axis=1)
    else:
        wide = r.tok_in[...].astype(f32)

    def nothing():
        pass

    def turn_keys(lower, upper):
        kc, kt = r.kc, r.kt

        def one(b, carry):
            kt[b] = kc[b].T
            return carry

        lax.fori_loop(lower, upper, one, 0, unroll=2)

    def first_fill():
        flat = positions * heads
        row_head = lax.rem(lax.broadcasted_iota(jnp.int32, (2 * heads, flat), 0), heads)
        column = lax.broadcasted_iota(jnp.int32, (2 * heads, flat), 1)
        r.pos[...] = jnp.where(
            lax.rem(column, heads) == row_head,
            column // heads + me_k * positions,
            jnp.int32(2**30),
        )
        pick_row = lax.broadcasted_iota(jnp.int32, (LANE, 4 * LANE), 0)
        pick_block = lax.broadcasted_iota(jnp.int32, (LANE, 4 * LANE), 1) // LANE
        r.pick[...] = jnp.where(pick_row // 3 == pick_block, 1.0, 0.0).astype(bf16)

        if cfg.turned:
            finish(loads.kc)
            turn_keys(0, rows)
        for ref in (r.g2, r.u2):
            if ref.shape[1] > units:
                ref[:, units:] = jnp.zeros((ref.shape[0], ref.shape[1] - units), bf16)
        for ref in (r.d1, r.d2):
            if ref.shape[0] > units:
                ref[units:, :] = jnp.zeros((ref.shape[0] - units, ref.shape[1]), bf16)

    part = gated(
        wide,
        0,
        r.g1,
        r.u1,
        r.d1,
        loads.d1,
        r.gu_send1,
        r.gu_recv1,
        r.gu_sem1,
        r.hid1,
        r.hid_sem1,
        first_fill,
    )
    first = (wide + 0.5 * tp_total(part, r.down1, r.down_sem1.at[0])).astype(bf16).astype(f32)

    finish(loads.wq)
    scaled = scaled_by(first, 1)
    q_send, q_recv, q_sem = r.q_send, r.q_recv, r.q_sem
    halves = 2 if heads % 2 == 0 else 1
    half_inner = inner // halves
    for side in range(halves):
        cut = pl.ds(side * half_inner, half_inner)
        query_part = dot(scaled, r.wq[:, cut]).astype(bf16)
        for c in range(chunks):
            q_send[c, :, cut] = query_part[c * chunk : (c + 1) * chunk]
        if side < halves - 1:
            starts = [
                (q_send.at[0, :, cut], q_recv.at[me_k, 0, :, cut], kv_partner[i], None)
                for i in far_first
            ]
            ship(starts, q_sem.at[0], "kv", len(groups))
    for c in range(chunks):
        cut = pl.ds((halves - 1) * half_inner, half_inner) if c == 0 else pl.ds(0, inner)
        own = ship(
            [
                (q_send.at[c, :, cut], q_recv.at[me_k, c, :, cut], kv_partner[i], None)
                for i in far_first
            ],
            q_sem.at[c],
            "kv",
        )
        sent(own, q_recv.at[pl.ds(0, n - 1), c])
        if c == 0:
            send_squares(first, 1)

    kv_send, kv_recv, kv_sem = r.kv_send, r.kv_recv, r.kv_sem
    finish(loads.wk, loads.wv)
    key_part = dot(scaled, r.wk[...]).astype(bf16)
    value_part = dot(scaled, r.wv[...]).astype(bf16)
    shift = jnp.where(me_k < n // 2, owners // 2, 0)
    my_place = me_k - first_owner
    is_owner = jnp.logical_and(my_place >= 0, my_place < owners)
    my_slot = jnp.clip(my_place, 0, owners - 1)
    for j in range(owners):
        kv_send[j, :, :share] = key_part[:, j * share : (j + 1) * share]
        kv_send[j, :, share:] = value_part[:, j * share : (j + 1) * share]
    owner_order = [lax.rem(j + shift, owners) for j in range(owners)]

    def to_owners(source, target, sem):
        own = ship(
            [
                (source.at[j], target, j + first_owner, me_k != j + first_owner)
                for j in owner_order
            ],
            sem,
            "kv",
        )
        if owners > 1:
            sent(own, source.at[pl.ds(0, owners - 1)], is_owner)
        sent(own, source.at[pl.ds(0, owners)], jnp.logical_not(is_owner))

    to_owners(kv_send, kv_recv.at[me_k], kv_sem.at[0])

    inv = inverse(1)
    logit_scale = HEAD_DIM ** (-0.5)
    wide_lane = lax.broadcasted_iota(jnp.int32, (2 * heads, LANE), 1)
    third = lax.rem(wide_lane, 3)
    map_row = lax.broadcasted_iota(jnp.int32, (2 * heads, LANE), 0) // heads
    slot = wide_lane - 6 * map_row
    first_half = lax.broadcasted_iota(jnp.int32, (chunk, LANE), 1) < HEAD_DIM
    finish(loads.vc)
    if not cfg.turned:
        finish(loads.kc)
    kc, vc, kt, qf, acc, q_all = r.kc, r.vc, r.kt, r.qf, r.acc, r.q_all
    score_ref, pos, lengths = r.score, r.pos, r.lengths
    att_send, att_recv, part_sem = r.att_send, r.att_recv, r.part_sem

    def attend(c):
        q_recv[me_k, c] = q_send[c]
        arrive(q_recv.at[pl.ds(0, n - 1), c], q_sem.at[c])
        total = q_recv[0, c].astype(f32)
        for source in range(1, n):
            total += q_recv[source, c].astype(f32)
        query = (total * inv[c * chunk : (c + 1) * chunk]).astype(bf16)
        q_all[c * chunk : (c + 1) * chunk, :] = query.astype(f32)
        for h in range(heads):
            block = query[:, h * VAL_DIM : (h + 1) * VAL_DIM].astype(f32) * logit_scale
            qf[:, h, :] = jnp.where(first_half, block, 0.0)
            qf[:, heads + h, :] = jnp.where(first_half, 0.0, block)
        for i in range(chunk):
            b = c * chunk + i
            if cfg.turned:
                score_ref[i] = dot(qf[i].astype(bf16), kt[b])
            else:
                score_ref[i] = lax.dot_general(
                    qf[i].astype(bf16),
                    kc[b],
                    (((1,), (1,)), ((), ())),
                    preferred_element_type=f32,
                )
        for i in range(chunk):
            b = c * chunk + i
            score = jnp.where(pos[...] < lengths[b], score_ref[i], neg_fill)
            peak = jnp.max(score, axis=1, keepdims=True)
            weight = jnp.exp(score - peak)
            mass = jnp.sum(weight, axis=1, keepdims=True)
            acc[i, :, :LANE] = dot(weight.astype(bf16), vc[b])
            stats = jnp.where(
                slot < 0, 0.0, jnp.where(slot < 3, peak, jnp.where(slot < 6, mass, 0.0))
            )
            high = stats.astype(bf16).astype(f32)
            mid = (stats - high).astype(bf16).astype(f32)
            low = stats - high - mid
            acc[i, :, LANE:] = jnp.where(third == 0, high, jnp.where(third == 1, mid, low))
        for j in range(owners):
            for p in range(per):
                head = j * per + p
                one, two = acc[:, head, :], acc[:, heads + head, :]
                place = pl.ds(p * chunk, chunk)
                att_send[c, j, place, :LANE] = one[:, :LANE].astype(bf16)
                att_send[c, j, place, LANE : 2 * LANE] = two[:, :LANE].astype(bf16)
                att_send[c, j, place, 2 * LANE :] = (one[:, LANE:] + two[:, LANE:]).astype(bf16)
        to_owners(att_send.at[c], att_recv.at[me_k, c], part_sem.at[c])

    for c in range(chunks):
        attend(c)

    att_all, att_sem = r.att_all, r.att_sem
    my_share = lanes(my_slot * share, share)
    half = lax.broadcasted_iota(jnp.int32, (per * chunk, LANE), 1) < HEAD_DIM

    def combine():
        kv_recv[me_k] = kv_send[my_slot]
        arrive(kv_recv.at[pl.ds(0, n - 1)], kv_sem.at[0])
        fresh = kv_recv[0].astype(f32)
        for source in range(1, n):
            fresh += kv_recv[source].astype(f32)
        fresh = (fresh * inv).astype(bf16).astype(f32)
        fresh_key, fresh_value = fresh[:, :share], fresh[:, share:]
        query = q_all[:, my_share]
        product = query * fresh_key * logit_scale

        def stacked(x, c):
            return jnp.concatenate(
                [
                    x[c * chunk : (c + 1) * chunk, p * VAL_DIM : (p + 1) * VAL_DIM]
                    for p in range(per)
                ],
                axis=0,
            )

        own = []
        for c in range(chunks):
            block = stacked(product, c)
            own.append(
                [
                    jnp.sum(jnp.where(half, block, 0.0), axis=1, keepdims=True),
                    jnp.sum(jnp.where(half, 0.0, block), axis=1, keepdims=True),
                ]
            )
        lam_rows = jnp.concatenate(
            [jnp.full((chunk, LANE), r.lam[my_slot * per + p], f32) for p in range(per)], axis=0
        )
        for c in range(chunks):
            att_recv[me_k, c] = att_send[c, my_slot]
            arrive(att_recv.at[pl.ds(0, n - 1), c], part_sem.at[c])
            stats = jnp.concatenate(
                [att_recv[source, c, :, 2 * LANE :] for source in range(n)], axis=0
            )
            stats = dot(stats, r.pick[...])
            high = per * chunk
            new_value = stacked(fresh_value, c)
            maps = []
            for m in range(2):
                peaks = [
                    stats[s * high : (s + 1) * high, 2 * m * LANE : (2 * m + 1) * LANE]
                    for s in range(n)
                ]
                masses = [
                    stats[s * high : (s + 1) * high, (2 * m + 1) * LANE : (2 * m + 2) * LANE]
                    for s in range(n)
                ]
                highest = jnp.broadcast_to(own[c][m], (high, LANE))
                for peak in peaks:
                    highest = jnp.maximum(highest, peak)
                own_weight = jnp.exp(own[c][m] - highest)
                den = own_weight
                num = own_weight.astype(bf16).astype(f32) * new_value
                for source in range(n):
                    scale = jnp.exp(peaks[source] - highest)
                    den += scale * masses[source]
                    num += scale * att_recv[source, c, :, m * LANE : (m + 1) * LANE].astype(f32)
                maps.append(num / den)
            mixed = maps[0] - lam_rows * maps[1]
            normed = (
                mixed
                * lax.rsqrt(jnp.mean(mixed * mixed, axis=1, keepdims=True) + epsilon)
                * r.head_gain[...]
            )
            for p in range(per):
                r.att_own[c * chunk : (c + 1) * chunk, p * VAL_DIM : (p + 1) * VAL_DIM] = (
                    normed[p * chunk : (p + 1) * chunk]
                )
        att_all[:, my_share] = r.att_own[...].astype(bf16)

    pl.when(is_owner)(combine)
    att_halves = halved and owners % 2 == 0 and 2 * first_owner + owners == n
    own = r.send_sem.at[len(groups)]
    groups.append(n - 1)
    for i in far_first:
        copy = pltpu.make_async_remote_copy(
            src_ref=att_all.at[:, my_share],
            dst_ref=att_all.at[:, my_share],
            send_sem=own,
            recv_sem=att_sem.at[1 if att_halves and i >= n // 2 else 0],
            device_id=(kv_partner[i], me_t),
            device_id_type=MESH,
        )
        when(is_owner, copy.start)
    sent(own, kv_recv.at[pl.ds(0, n - 1), :, pl.ds(0, share)], is_owner)
    finish(loads.wo)

    def att_arrive(index, count):
        if count:
            arrive(att_all.at[:, pl.ds(0, count * share)], att_sem.at[index])

    def att_arrive_near(count):
        pl.when(is_owner)(lambda: att_arrive(0, count - 1))
        pl.when(jnp.logical_not(is_owner))(lambda: att_arrive(0, count))

    wo = r.wo
    if att_halves:
        size = owners // 2 * share
        near = jnp.where(me_k < n // 2, 0, size)
        att_arrive_near(owners // 2)
        part = dot(att_all[:, lanes(near, size)], wo[lanes(near, size), :])
        att_arrive(1, owners // 2)
        far = size - near
        part += dot(att_all[:, lanes(far, size)], wo[lanes(far, size), :])
    else:
        att_arrive_near(owners)
        part = dot(att_all[...], wo[...])
    second = (first + tp_total(part, r.out_all, r.out_sem.at[0])).astype(bf16).astype(f32)

    finish(loads.g2, loads.u2)
    stream, result = r.stream, r.result
    stream[...] = second
    part = gated(
        second,
        2,
        r.g2,
        r.u2,
        r.d2,
        loads.d2,
        r.gu_send2,
        r.gu_recv2,
        r.gu_sem2,
        r.hid2,
        r.hid_sem2,
        nothing,
    )
    if gather_here:
        down2, down2_recv, sem = r.down2, r.down2_recv, r.down_sem2.at[0]
        for s in range(t):
            down2[s] = part[:, s * cols : (s + 1) * cols].astype(bf16)
        own = ship(
            [(down2.at[peer], down2_recv.at[me_t], peer, None) for peer in tp_partner[:0:-1]],
            sem,
            "tp",
        )
        sent(own, down2.at[pl.ds(0, t - 1)])
        down2_recv[me_t] = down2[me_t]
        tp_await(down2_recv, sem)
        total = down2_recv[0].astype(f32)
        for source in range(1, t):
            total += down2_recv[source].astype(f32)
        own = stream[:, lanes(me_t * cols, cols)]
        result[...] = (own + 0.5 * total).astype(bf16)
    else:
        total = tp_total(part, r.down2, r.down_sem2.at[0])
        result[...] = (second + 0.5 * total).astype(bf16)
    for copy, condition in sends:
        when(condition, copy.wait_send)


def on_device(
    tokens,
    first_gain,
    first_gate,
    first_up,
    first_down,
    mixer_gain,
    w_query,
    w_key,
    w_value,
    w_output,
    lam_heads,
    head_gain,
    key_cache,
    value_cache,
    lengths,
    last_gain,
    last_gate,
    last_up,
    last_down,
):
    n, t = lax.axis_size("kv"), lax.axis_size("tp")
    rows, cols = tokens.shape
    width, units = first_gate.shape
    positions, heads = key_cache.shape[1:3]
    gather_here = cols % LANE == 0
    tiles = ceil_div(units, LANE)
    base, rem = divmod(tiles, n)
    lo = (n - rem) // 2
    owners = heads // 2 if heads % 2 == 0 and heads // 2 <= n else heads
    per = heads // owners
    chunks = 2 if rows % 16 == 0 else 1
    chunk = rows // chunks
    inner = heads * VAL_DIM
    share = per * VAL_DIM
    cfg = types.SimpleNamespace(
        n=n,
        t=t,
        model=width * n,
        rows=rows,
        cols=cols,
        units=units,
        heads=heads,
        positions=positions,
        tiles=tiles,
        base=base,
        rem=rem,
        lo=lo,
        owners=owners,
        per=per,
        first_owner=(n - owners) // 2,
        gather_here=gather_here,
        chunks=chunks,
        chunk=chunk,
        turned=TURNED,
    )
    if not gather_here:
        tokens = lax.all_gather(tokens, "tp", axis=1, tiled=True)
    flat = positions * heads
    keys = key_cache.reshape(rows, flat, VAL_DIM)
    values = value_cache.reshape(rows, flat, VAL_DIM)

    wide_units = (tiles + (1 if rem else 0)) * LANE
    gu = (n, rows, 2 * (base + (1 if rem else 0)) * LANE)
    dma = pltpu.SemaphoreType.DMA
    return_cols = cols if gather_here else width
    inputs = dict(
        tokens=tokens,
        gain0_in=first_gain.reshape(1, width),
        gain1_in=mixer_gain.reshape(1, width),
        gain2_in=last_gain.reshape(1, width),
        head_gain_in=head_gain.reshape(1, VAL_DIM),
        lam_in=lam_heads,
        lengths_in=lengths,
        first_gate=first_gate,
        first_up=first_up,
        first_down=first_down,
        w_query=w_query,
        w_key=w_key,
        w_value=w_value,
        w_output=w_output,
        keys=keys,
        values=values,
        last_gate=last_gate,
        last_up=last_up,
        last_down=last_down,
    )
    scratch = dict(
        gain0=((1, width), f32),
        gain1=((1, width), f32),
        gain2=((1, width), f32),
        head_gain=((1, VAL_DIM), f32),
        g1=((width, wide_units), bf16),
        u1=((width, wide_units), bf16),
        d1=((tiles * LANE, width), bf16),
        wq=((width, inner), bf16),
        wk=((width, inner), bf16),
        wv=((width, inner), bf16),
        wo=((inner, width), bf16),
        kc=((rows, flat, VAL_DIM), bf16),
        vc=((rows, flat, VAL_DIM), bf16),
        kt=((rows, VAL_DIM, flat) if TURNED else (1, VAL_DIM, LANE), bf16),
        g2=((width, wide_units), bf16),
        u2=((width, wide_units), bf16),
        d2=((tiles * LANE, width), bf16),
        stream=((rows, width), f32),
        squares=((3, n, 1, LANE), f32),
        gu_send1=(gu, bf16),
        gu_recv1=(gu, bf16),
        gu_send2=(gu, bf16),
        gu_recv2=(gu, bf16),
        hid1=((rows, wide_units), bf16),
        hid2=((rows, wide_units), bf16),
        down1=((t, rows, width), bf16),
        out_all=((t, rows, width), bf16),
        q_send=((chunks, chunk, inner), bf16),
        q_recv=((n, chunks, chunk, inner), bf16),
        q_all=((rows, inner), f32),
        kv_send=((owners, rows, 2 * share), bf16),
        kv_recv=((n, rows, 2 * share), bf16),
        qf=((chunk, 2 * heads, VAL_DIM), f32),
        score=((chunk, 2 * heads, flat), f32),
        acc=((chunk, 2 * heads, VAL_DIM + LANE), f32),
        pos=((2 * heads, flat), jnp.int32),
        pick=((LANE, 4 * LANE), bf16),
        att_send=((chunks, owners, per * chunk, 2 * VAL_DIM + LANE), bf16),
        att_recv=((n, chunks, per * chunk, 2 * VAL_DIM + LANE), bf16),
        att_own=((rows, share), f32),
        att_all=((rows, inner), bf16),
    )
    if gather_here:
        scratch.update(
            tok_all=((t, rows, cols), bf16),
            down2=((t, rows, cols), bf16),
            down2_recv=((t, rows, cols), bf16),
        )
    else:
        scratch.update(tok_in=((rows, width), bf16), down2=((t, rows, width), bf16))
    sems = dict(
        load_sem=(19,),
        send_sem=(3 + 8 + 2 * chunks + 2 + 4,),
        tok_sem=(1,),
        sq_sem=(3,),
        gu_sem1=(2,),
        gu_sem2=(2,),
        hid_sem1=(2,),
        hid_sem2=(2,),
        down_sem1=(1,),
        down_sem2=(1,),
        out_sem=(1,),
        q_sem=(chunks,),
        kv_sem=(1,),
        part_sem=(chunks,),
        att_sem=(2,),
    )
    smem = dict(lam=(lam_heads.shape, f32), lengths=(lengths.shape, jnp.int32))
    names = [*inputs, *dict(result=0), *scratch, *smem, *sems, *dict(greet_sem=0)]
    result = pl.pallas_call(
        functools.partial(layer_kernel, cfg, names),
        out_shape=pltpu.VMEM((rows, return_cols), bf16),
        in_specs=[pl.BlockSpec(memory_space=pl.ANY)] * len(inputs),
        out_specs=pl.BlockSpec(memory_space=pltpu.VMEM),
        scratch_shapes=[pltpu.VMEM(shape, kind) for shape, kind in scratch.values()]
        + [pltpu.SMEM(shape, kind) for shape, kind in smem.values()]
        + [dma(shape) for shape in sems.values()]
        + [pltpu.SemaphoreType.REGULAR((2,))],
        compiler_params=pltpu.CompilerParams(
            collective_id=0, has_side_effects=True, vmem_limit_bytes=63 * 2**20
        ),
    )(*inputs.values())
    if not gather_here:
        result = lax.dynamic_slice_in_dim(result, lax.axis_index("tp") * cols, cols, 1)
    return result


TURNED = True


def solution(mesh):
    return jax.shard_map(
        on_device,
        mesh=mesh,
        in_specs=(
            P(None, ("kv", "tp")),
            P("kv"),
            P("kv", "tp"),
            P("kv", "tp"),
            P("tp", "kv"),
            P("kv"),
            P("kv", "tp"),
            P("kv", "tp"),
            P("kv", "tp"),
            P("tp", "kv"),
            P("tp"),
            P(),
            P(None, "kv", "tp", None),
            P(None, "kv", "tp", None),
            P(),
            P("kv"),
            P("kv", "tp"),
            P("kv", "tp"),
            P("tp", "kv"),
        ),
        out_specs=P(None, ("kv", "tp")),
        check_vma=False,
    )
```
